32 devices in a mesh: sp: 8 (over z, y), tp: 4 (over x, core).
Axes of the slice: x: 2, y: 2, z: 4, core: 2. Of those that a mesh axis runs over, the one named last changes fastest.
Arguments:
- hidden: bfloat16 [3072, 4096], P('sp', 'tp'), may hold values from -6 to 6
- doc_ids: int32 [3072], P('sp'), may hold values from 0 to 3, never falling along the last dimension, each value on 1 to 1536 neighbouring positions
- norm_gain: float32 [3, 4096], replicated, may hold values from 0.1 to 1.9
- w_value: bfloat16 [3, 4096, 2048], P(None, 'sp', 'tp'), may hold values from -0.09375 to 0.09375
- w_gate: bfloat16 [3, 4096, 2048], P(None, 'sp', 'tp'), may hold values from -0.09375 to 0.09375
- conv_taps: float32 [3, 31, 2048], P(None, None, 'tp'), may hold values from -1 to 1
- conv_bias: float32 [3, 2048], P(None, 'tp'), may hold values from -3 to 3
- chan_gain: float32 [3, 2048], P(None, 'tp'), may hold values from 0.1 to 1.9
- chan_bias: float32 [3, 2048], P(None, 'tp'), may hold values from -3 to 3
- w_out: bfloat16 [3, 2048, 4096], P(None, 'sp', 'tp'), may hold values from -0.125 to 0.125
Outputs:
- result: bfloat16 [3072, 4096], P('sp', 'tp')
The draws below stay inside these ranges and needn't reach their ends.
Inputs may be any that keep to these rules, and one draw needn't show every extreme that they name: `doc_ids`: document numbers never fall along the sequence; each document has 1 to 1536 positions and one has exactly that many.
All inputs are finite; a program needn't handle non-finite values.
Results may differ from the reference program's by a relative error of at most 0.013.
Values may be sent and summed in bfloat16 or wider, within the bound.
A program may use at most 128 MiB of HBM per device.

```python
import math
import jax
import jax.numpy as jnp
import numpy as np
from jax import lax

D = 4096
C = 2048
CONV_WIDTH = 31
LAYERS = 3
TOK_DEV = 384
TOKENS = 3072
DOCS = 4


def levels(own_key, extent, shards, low, largest):
    level = 1.0
    for position, shards_of in shards:
        steps = jax.random.uniform(jax.random.fold_in(jax.random.fold_in(own_key, 6), position), (shards_of,), jnp.float32, low / len(shards), largest / len(shards))
        level = level * jnp.repeat(jnp.exp(steps), extent[position] // shards_of).reshape((-1,) + (1,) * (len(extent) - 1 - position))
    return level


def profile(count, total, most, lean):
    loads = [(1 << 20) // math.isqrt(grade ** lean) + 1 for grade in range(2, count + 1)]
    rest, counts = total - most - (count - 1), [1] * (count - 1)
    while rest > 0:
        free = [i for i in range(count - 1) if counts[i] < most]
        mass, left = sum([loads[i] for i in free]), rest
        for i in free:
            more = min(most - counts[i], max(1, left * loads[i] // mass), rest)
            counts[i] = counts[i] + more
            rest = rest - more
    return np.array([most] + counts)


def uneven_parts(stream_key, amount, total, limit, lean):
    if amount == 2:
        one = jax.random.randint(stream_key, (), max(1, total - limit), min(limit, total - 1) + 1)
        return jnp.stack([one, total - one])
    lengths = jnp.asarray(profile(amount, total, limit, lean), jnp.int32)
    twos = (amount - 1) // 2
    donor, taker = lengths[1:1 + 2 * twos:2], lengths[2:2 + 2 * twos:2]
    margin = jnp.minimum(donor - 1, limit - taker)
    passed = jax.random.randint(jax.random.fold_in(stream_key, 1), (twos,), 0, 1 << 20) % (margin + 1)
    lengths = lengths.at[1:1 + 2 * twos:2].set(donor - passed).at[2:2 + 2 * twos:2].set(taker + passed)
    return lengths[jax.random.permutation(jax.random.fold_in(stream_key, 2), amount)]


def scatter_about(own_key, shape, scale, reach, pieces=(), dtype=jnp.bfloat16):
    loudness = levels(own_key, shape, pieces, -0.22, 0.18) if pieces else 1.0
    drawn = jax.random.normal(own_key, shape, jnp.float32) * scale * loudness
    return jnp.minimum(jnp.maximum(drawn, -reach), reach).astype(dtype)


def setup_inputs(seed: int = 0) -> dict:
    arg_keys = jax.random.split(jax.random.key(seed), 11)
    hidden = scatter_about(arg_keys[0], (TOKENS, D), 1.0, 6.0, ((0, 8), (1, 4)))
    doc_ids = jnp.searchsorted(jnp.cumsum(uneven_parts(arg_keys[1], DOCS, TOKENS, 4 * TOK_DEV, 0)), jnp.arange(TOKENS), side="right").astype(jnp.int32)
    norm_gain = jnp.clip(1.0 + 0.18 * jax.random.normal(arg_keys[2], (LAYERS, D), jnp.float32), 0.1, 1.9)
    w_value = scatter_about(arg_keys[3], (LAYERS, D, C), D ** -0.5, 0.09375, ((1, 8), (2, 4)))
    w_gate = scatter_about(arg_keys[4], (LAYERS, D, C), D ** -0.5, 0.09375, ((1, 8), (2, 4)))
    conv_taps = scatter_about(arg_keys[5], (LAYERS, CONV_WIDTH, C), CONV_WIDTH ** -0.5, 1.0, ((2, 4),), jnp.float32)
    conv_bias = scatter_about(arg_keys[6], (LAYERS, C), 0.5, 3.0, ((1, 4),), jnp.float32)
    chan_gain = jnp.clip(1.0 + 0.18 * jax.random.normal(arg_keys[7], (LAYERS, C), jnp.float32), 0.1, 1.9)
    chan_bias = scatter_about(arg_keys[8], (LAYERS, C), 0.5, 3.0, ((1, 4),), jnp.float32)
    w_out = scatter_about(arg_keys[9], (LAYERS, C, D), C ** -0.5, 0.125, ((1, 8), (2, 4)))
    return {"hidden": hidden, "doc_ids": doc_ids, "norm_gain": norm_gain, "w_value": w_value, "w_gate": w_gate, "conv_taps": conv_taps, "conv_bias": conv_bias, "chan_gain": chan_gain, "chan_bias": chan_bias, "w_out": w_out}


def one_layer(hidden, doc_ids, norm_gain, w_value, w_gate, conv_taps, conv_bias, chan_gain, chan_bias, w_out):
    width = conv_taps.shape[0]
    length = hidden.shape[0]
    xfloat = hidden.astype(jnp.float32)
    scale = lax.rsqrt(lax.optimization_barrier(jnp.mean(xfloat * xfloat, axis=-1, keepdims=True)) + 1e-06)
    normed = (xfloat * scale * norm_gain).astype(jnp.bfloat16)
    value = jnp.dot(normed, w_value, preferred_element_type=jnp.float32)
    gate = jnp.dot(normed, w_gate, preferred_element_type=jnp.float32)
    glu = (value * jax.nn.sigmoid(gate)).astype(jnp.bfloat16)
    padded = jnp.concatenate([jnp.zeros((width - 1, glu.shape[1]), jnp.float32), glu.astype(jnp.float32)], axis=0)
    seg_pad = jnp.concatenate([jnp.full((width - 1,), -1, jnp.int32), doc_ids.astype(jnp.int32)], axis=0)
    conv = jnp.zeros(glu.shape, jnp.float32) + conv_bias
    for index in range(width):
        source = padded[index:index + length]
        keep = (seg_pad[index:index + length] == doc_ids)[:, None]
        conv = conv + jnp.where(keep, source * conv_taps[index], 0.0)
    mean_val = lax.optimization_barrier(jnp.mean(conv, axis=-1, keepdims=True))
    var_val = lax.optimization_barrier(jnp.mean(conv * conv, axis=-1, keepdims=True)) - mean_val * mean_val
    mixed = jax.nn.silu((conv - mean_val) * lax.rsqrt(var_val + 1e-05) * chan_gain + chan_bias).astype(jnp.bfloat16)
    return (xfloat + jnp.dot(mixed, w_out, preferred_element_type=jnp.float32)).astype(jnp.bfloat16)

def reference(hidden, doc_ids, norm_gain, w_value, w_gate, conv_taps, conv_bias, chan_gain, chan_bias, w_out):
    state = hidden
    for layer in range(LAYERS):
        state = one_layer(state, doc_ids, norm_gain[layer], w_value[layer], w_gate[layer], conv_taps[layer], conv_bias[layer], chan_gain[layer], chan_bias[layer], w_out[layer])
    return state
```

```python
import math

import jax
import jax.numpy as jnp
from jax import lax
from jax.sharding import PartitionSpec as P

LAYERS = 3


def from_behind(shard, axis, by):
    size = lax.axis_size(axis)
    pairs = [(i, i + by) for i in range(size) if 0 <= i + by < size]
    return lax.ppermute(shard, axis, pairs)


def grid_of(size):
    inner = max(d for d in range(1, math.isqrt(size) + 1) if size % d == 0)
    return size // inner, inner


def line_gather(block, size, stride, other):
    where = (lax.axis_index("sp") // stride) % size
    bases = (
        [o for o in range(stride)] if stride > 1 else [o * size for o in range(other)]
    )

    def hop(shard, moves):
        return lax.ppermute(
            shard, "sp", [(b + i * stride, b + j * stride) for b in bases for i, j in moves]
        )

    if size == 1:
        return [block]
    if size == 2:
        return [block, hop(block, [(0, 1), (1, 0)])]
    down, up = [block], [block]
    for step in range(1, size):
        down.append(hop(down[-1], [(i, i - 1) for i in range(1, size - step + 1)]))
        up.append(hop(up[-1], [(i, i + 1) for i in range(step - 1, size - 1)]))
    return [block] + [
        jnp.where(where + d < size, down[d], up[size - d]) for d in range(1, size)
    ]


def grid_gather(block, outer_first):
    depth, inner = grid_of(lax.axis_size("sp"))
    me = lax.axis_index("sp")
    z, y = me // inner, me % inner
    found = []
    if outer_first:
        for dz, slot in enumerate(line_gather(block, depth, inner, depth)):
            for dy, piece in enumerate(line_gather(slot, inner, 1, depth)):
                found.append((((z + dz) % depth) * inner + (y + dy) % inner, piece))
    else:
        for dy, slot in enumerate(line_gather(block, inner, 1, depth)):
            for dz, piece in enumerate(line_gather(slot, depth, inner, depth)):
                found.append((((z + dz) % depth) * inner + (y + dy) % inner, piece))
    return found


def blocks_dot(rows, pieces):
    total = None
    for origin, piece in pieces:
        depth = piece.shape[0]
        part = jnp.dot(
            lax.dynamic_slice_in_dim(rows, origin * depth, depth, axis=1),
            piece,
            preferred_element_type=jnp.float32,
        )
        total = part if total is None else total + part
    return total


def per_device(
    hidden, doc_ids, norm_gain, w_value, w_gate, conv_taps, conv_bias, chan_gain, chan_bias, w_out
):
    width = conv_taps.shape[1]
    length = hidden.shape[0]
    chan_local = w_value.shape[2]
    chan_total = chan_local * lax.axis_size("tp")
    seg_own = doc_ids + 1
    halo_seg = from_behind(seg_own[length - (width - 1) :], "sp", 1)
    seg_ext = jnp.concatenate([halo_seg, seg_own], axis=0)
    proj, outs = [], []
    for layer in range(LAYERS):
        both = jnp.concatenate([w_value[layer], w_gate[layer]], axis=1)
        proj.append(grid_gather(both, True))
        outs.append(grid_gather(w_out[layer], layer < LAYERS - 1))
    state = hidden
    for layer in range(LAYERS):
        whole = lax.all_gather(state, "tp", axis=1, tiled=True)
        xwhole = whole.astype(jnp.float32)
        scale = lax.rsqrt(jnp.mean(xwhole * xwhole, axis=-1, keepdims=True) + 1e-06)
        normed = (xwhole * scale * norm_gain[layer]).astype(jnp.bfloat16)
        product = blocks_dot(normed, proj[layer])
        value, gate = product[:, :chan_local], product[:, chan_local:]
        glu = (value * jax.nn.sigmoid(gate)).astype(jnp.bfloat16)
        halo_glu = from_behind(glu[length - (width - 1) :], "sp", 1)
        extended = jnp.concatenate([halo_glu, glu], axis=0).astype(jnp.float32)
        taps = conv_taps[layer]
        conv = jnp.zeros((length, chan_local), jnp.float32) + conv_bias[layer]
        for index in range(width):
            keep = (seg_ext[index : index + length] == seg_own)[:, None]
            conv = conv + jnp.where(keep, extended[index : index + length] * taps[index], 0.0)
        total, square = lax.psum((jnp.sum(conv, axis=-1), jnp.sum(conv * conv, axis=-1)), "tp")
        mean_val = (total / chan_total)[:, None]
        var_val = (square / chan_total)[:, None] - mean_val * mean_val
        mixed = jax.nn.silu(
            (conv - mean_val) * lax.rsqrt(var_val + 1e-05) * chan_gain[layer] + chan_bias[layer]
        ).astype(jnp.bfloat16)
        mixed_all = lax.all_gather(mixed, "tp", axis=1, tiled=True)
        branch = blocks_dot(mixed_all, outs[layer])
        state = (state.astype(jnp.float32) + branch).astype(jnp.bfloat16)
    return state


def solution(mesh):
    placed = (
        P("sp", "tp"),
        P("sp"),
        P(),
        P(None, "sp", "tp"),
        P(None, "sp", "tp"),
        P(None, None, "tp"),
        P(None, "tp"),
        P(None, "tp"),
        P(None, "tp"),
        P(None, "sp", "tp"),
    )
    return jax.shard_map(
        per_device, mesh=mesh, in_specs=placed, out_specs=P("sp", "tp"), check_vma=False
    )
```

```python
import math

import jax
import jax.numpy as jnp
from jax import lax
from jax.sharding import PartitionSpec as P

LAYERS = 3


def from_behind(shard, axis, by):
    size = lax.axis_size(axis)
    pairs = [(i, i + by) for i in range(size) if 0 <= i + by < size]
    return lax.ppermute(shard, axis, pairs)


def grid_of(size):
    inner = max(d for d in range(1, math.isqrt(size) + 1) if size % d == 0)
    return size // inner, inner


WINDOW = 2


def tie(value, *earlier):
    return lax.optimization_barrier((value,) + earlier)[0] if earlier else value


class Lane:
    def __init__(self):
        self.done = []

    def hop(self, shard, pairs):
        moved = lax.ppermute(tie(shard, *self.done[-WINDOW : len(self.done) - WINDOW + 1]), "sp", pairs)
        self.done.append(moved)
        return moved


class Line:
    def __init__(self, size, stride, total):
        self.size, self.stride = size, stride
        self.where = (lax.axis_index("sp") // stride) % size
        self.bases = [i for i in range(total) if (i // stride) % size == 0]
        self.down, self.up = Lane(), Lane()

    def pairs(self, moves):
        s = self.stride
        return [(b + i * s, b + j * s) for b in self.bases for i, j in moves]

    def gather(self, block):
        size = self.size
        if size == 1:
            return [block]
        if size == 2:
            return [block, self.down.hop(block, self.pairs([(0, 1), (1, 0)]))]
        down, up = [block], [block]
        for step in range(1, size):
            down.append(
                self.down.hop(
                    down[-1], self.pairs([(i, i - 1) for i in range(1, size - step + 1)])
                )
            )
            up.append(
                self.up.hop(up[-1], self.pairs([(i, i + 1) for i in range(step - 1, size - 1)]))
            )
        return [block] + [
            jnp.where(self.where + d < size, down[d], up[size - d]) for d in range(1, size)
        ]

    def last(self):
        return [lane.done[-1] for lane in (self.down, self.up) if lane.done]


def gather_all(proj, outs):
    total = lax.axis_size("sp")
    depth, inner = grid_of(total)
    me = lax.axis_index("sp")
    z, y = me // inner, me % inner
    far, near = Line(depth, inner, total), Line(inner, 1, total)

    def origin(dz, dy):
        return ((z + dz) % depth) * inner + (y + dy) % inner

    def own(block):
        return {(0, dy): piece for dy, piece in enumerate(near.gather(block))}

    def spread_near(found, slots):
        for dz in range(1, depth):
            for dy, piece in enumerate(near.gather(slots[dz])):
                found[dz, dy] = piece

    def spread_far(found):
        for dy in range(inner):
            for dz, piece in enumerate(far.gather(found[0, dy])):
                found[dz, dy] = piece

    marks = {}
    p0, o0, p1, o1 = own(proj[0]), own(outs[0]), own(proj[1]), own(outs[1])
    p0_far = far.gather(proj[0])
    o0_far = far.gather(outs[0])
    marks["proj0"] = far.last()
    p1_far = far.gather(proj[1])
    marks["out0"] = far.last()
    spread_near(p0, p0_far)
    spread_near(o0, o0_far)
    p2_far = far.gather(proj[2])
    marks["proj1"] = far.last()
    p2 = own(proj[2])
    marks["out0"] = marks["out0"] + near.last()
    spread_near(p1, p1_far)
    spread_far(o1)
    o2 = own(outs[2])
    marks["out1"] = near.last()
    spread_near(p2, p2_far)
    spread_far(o2)
    named = [
        [(origin(dz, dy), piece) for (dz, dy), piece in found.items()]
        for found in (p0, o0, p1, o1, p2, o2)
    ]
    return named[0::2], named[1::2], marks


def blocks_dot(rows, pieces):
    total = None
    for origin, piece in pieces:
        depth = piece.shape[0]
        part = jnp.dot(
            lax.dynamic_slice_in_dim(rows, origin * depth, depth, axis=1),
            piece,
            preferred_element_type=jnp.float32,
        )
        total = part if total is None else total + part
    return total


def per_device(
    hidden, doc_ids, norm_gain, w_value, w_gate, conv_taps, conv_bias, chan_gain, chan_bias, w_out
):
    width = conv_taps.shape[1]
    length = hidden.shape[0]
    chan_local = w_value.shape[2]
    chan_total = chan_local * lax.axis_size("tp")
    seg_own = doc_ids + 1
    halo_seg = from_behind(seg_own[length - (width - 1) :], "sp", 1)
    seg_ext = jnp.concatenate([halo_seg, seg_own], axis=0)
    proj, outs, marks = gather_all(
        [jnp.concatenate([w_value[layer], w_gate[layer]], axis=1) for layer in range(LAYERS)],
        [w_out[layer] for layer in range(LAYERS)],
    )
    state = hidden
    for layer in range(LAYERS):
        whole = lax.all_gather(state, "tp", axis=1, tiled=True)
        xwhole = whole.astype(jnp.float32)
        scale = lax.rsqrt(jnp.mean(xwhole * xwhole, axis=-1, keepdims=True) + 1e-06)
        normed = (xwhole * scale * norm_gain[layer]).astype(jnp.bfloat16)
        normed = tie(normed, *marks.get(f"proj{layer}", []))
        product = blocks_dot(normed, proj[layer])
        value, gate = product[:, :chan_local], product[:, chan_local:]
        glu = (value * jax.nn.sigmoid(gate)).astype(jnp.bfloat16)
        halo_glu = from_behind(glu[length - (width - 1) :], "sp", 1)
        extended = jnp.concatenate([halo_glu, glu], axis=0).astype(jnp.float32)
        taps = conv_taps[layer]
        conv = jnp.zeros((length, chan_local), jnp.float32) + conv_bias[layer]
        for index in range(width):
            keep = (seg_ext[index : index + length] == seg_own)[:, None]
            conv = conv + jnp.where(keep, extended[index : index + length] * taps[index], 0.0)
        total, square = lax.psum((jnp.sum(conv, axis=-1), jnp.sum(conv * conv, axis=-1)), "tp")
        mean_val = (total / chan_total)[:, None]
        var_val = (square / chan_total)[:, None] - mean_val * mean_val
        mixed = jax.nn.silu(
            (conv - mean_val) * lax.rsqrt(var_val + 1e-05) * chan_gain[layer] + chan_bias[layer]
        ).astype(jnp.bfloat16)
        mixed_all = lax.all_gather(mixed, "tp", axis=1, tiled=True)
        mixed_all = tie(mixed_all, *marks.get(f"out{layer}", []))
        branch = blocks_dot(mixed_all, outs[layer])
        state = (state.astype(jnp.float32) + branch).astype(jnp.bfloat16)
    return state


def solution(mesh):
    placed = (
        P("sp", "tp"),
        P("sp"),
        P(),
        P(None, "sp", "tp"),
        P(None, "sp", "tp"),
        P(None, None, "tp"),
        P(None, "tp"),
        P(None, "tp"),
        P(None, "tp"),
        P(None, "sp", "tp"),
    )
    return jax.shard_map(
        per_device, mesh=mesh, in_specs=placed, out_specs=P("sp", "tp"), check_vma=False
    )
```
